32 devices in a mesh: fs: 16 (over z, y, x), tp: 2 (over core).
Axes of the slice: x: 2, y: 2, z: 4, core: 2. Of those that a mesh axis runs over, the one named last changes fastest.
Arguments:
- tokens: bfloat16 [8192, 2048], P('fs'), may hold values from -6 to 6
- mixer_gain: float32 [2048], replicated, may hold values from 0.1 to 1.9
- w_query: bfloat16 [2048, 1024], P('fs', 'tp'), may hold values from -0.125 to 0.125
- w_key: bfloat16 [2048, 1024], P('fs', 'tp'), may hold values from -0.125 to 0.125
- w_value: bfloat16 [2048, 2048], P('fs', 'tp'), may hold values from -0.125 to 0.125
- gate_down: bfloat16 [2048, 32], replicated, may hold values from -0.125 to 0.125
- gate_up: bfloat16 [32, 1024], P(None, 'tp'), may hold values from -1 to 1
- decay_bias: float32 [1024], P('tp'), may hold values from -1 to 6
- decay_shift: float32 [8192, 8], P('fs', 'tp'), may hold values from -0.71 to 0, as said below
- head_gain: float32 [2048], P('tp'), may hold values from 0.1 to 1.9
- w_out: bfloat16 [2048, 2048], P('fs', 'tp'), may hold values from -0.125 to 0.125
- mlp_gain: float32 [2048], replicated, may hold values from 0.1 to 1.9
- mlp_up: bfloat16 [2048, 8192], P('fs', 'tp'), may hold values from -0.125 to 0.125
- mlp_down: bfloat16 [2048, 8192], P('fs', 'tp'), may hold values from -0.0625 to 0.0625
Outputs:
- layer_out: bfloat16 [8192, 2048], P('fs')
The draws below stay inside these ranges and needn't reach their ends.
Inputs may be any that keep to these rules, and one draw needn't show every extreme that they name: `decay_shift`: never positive.
All inputs are finite; a program needn't handle non-finite values.
Results may differ from the reference program's by a relative error of at most 0.022.
Values may be sent and summed in bfloat16 or wider, within the bound.
A program may use at most 128 MiB of HBM per device.

```python
import math
import jax
import jax.numpy as jnp
from jax import lax

D = 2048
ATTENTION_HEADS = 8
HEAD_K = 128
FF = 8192
RANK = 32
BLOCK_TOKENS = 64
SEQUENCE_LENGTH = 512
DK = 1024
DV = 2048
TOKENS = 8192
N_TP = 2


def draw_decay_bias(key, part):
    return jax.random.uniform(key, (ATTENTION_HEADS * HEAD_K,), jnp.float32, -1.0, 5.0)


def draw_decay_shift(key, part):
    decay_rate_key, jitter_random_key, spike_random_key, layer_depth_key = jax.random.split(jax.random.fold_in(key, 11), 4)
    every_block = TOKENS // BLOCK_TOKENS
    decay_rates = jnp.exp(jax.random.uniform(decay_rate_key, (every_block, 1, ATTENTION_HEADS), jnp.float32, math.log(0.0005), math.log(0.004)))
    random_jitter = jax.random.uniform(jitter_random_key, (every_block, BLOCK_TOKENS, ATTENTION_HEADS), jnp.float32, 0.0, 2.0)
    spike_values = jax.random.randint(spike_random_key, (every_block, BLOCK_TOKENS, ATTENTION_HEADS), 0, SEQUENCE_LENGTH) < 2
    layer_depth = jnp.log(jax.random.uniform(layer_depth_key, (every_block, BLOCK_TOKENS, ATTENTION_HEADS), jnp.float32, 0.5, 0.8))
    offset_amount = -decay_rates * random_jitter + jnp.where(spike_values, layer_depth, 0.0)
    return offset_amount.reshape(TOKENS, ATTENTION_HEADS).astype(jnp.float32)


def block_scale(stream_key, shape, cuts, least, largest):
    factor_of = 1.0
    for axis_at, blocks in cuts:
        steps = jax.random.uniform(jax.random.fold_in(jax.random.fold_in(stream_key, 6), axis_at), (blocks,), jnp.float32, least / len(cuts), largest / len(cuts))
        factor_of = factor_of * jnp.repeat(jnp.exp(steps), shape[axis_at] // blocks).reshape((-1,) + (1,) * (len(shape) - 1 - axis_at))
    return factor_of


def centred(key, extent, spread, bound, cuts=(), kind=jnp.bfloat16):
    result = jax.random.normal(key, extent, jnp.float32) * spread
    if len(cuts) > 0:
        result = block_scale(key, extent, cuts, -0.22, 0.18) * result
    return jnp.clip(result, min=-bound, max=bound).astype(kind)


def setup_inputs(seed: int = 0) -> dict:
    key_of = jax.random.split(jax.random.key(seed), 15)
    return {
        "tokens": centred(key_of[0], (TOKENS, D), 1.0, 6.0, ((0, 16),)),
        "mixer_gain": jnp.clip(1.0 + 0.18 * jax.random.normal(key_of[1], (D,), jnp.float32), 0.1, 1.9),
        "w_query": centred(key_of[2], (D, DK), D ** -0.5, 0.125, ((0, 16), (1, 2))),
        "w_key": centred(key_of[3], (D, DK), D ** -0.5, 0.125, ((0, 16), (1, 2))),
        "w_value": centred(key_of[4], (D, DV), D ** -0.5, 0.125, ((0, 16), (1, 2))),
        "gate_down": centred(key_of[5], (D, RANK), D ** -0.5, 0.125),
        "gate_up": centred(key_of[6], (RANK, DK), RANK ** -0.5, 1.0, ((1, 2),)),
        "decay_bias": draw_decay_bias(jax.random.fold_in(key_of[14], 71), 0),
        "decay_shift": draw_decay_shift(jax.random.fold_in(key_of[14], 71), 0),
        "head_gain": jnp.clip(1.0 + 0.18 * jax.random.normal(key_of[9], (DV,), jnp.float32), 0.1, 1.9),
        "w_out": centred(key_of[10], (D, DV), DV ** -0.5, 0.125, ((0, 16), (1, 2))),
        "mlp_gain": jnp.clip(1.0 + 0.18 * jax.random.normal(key_of[11], (D,), jnp.float32), 0.1, 1.9),
        "mlp_up": centred(key_of[12], (D, FF), D ** -0.5, 0.125, ((0, 16), (1, 2))),
        "mlp_down": centred(key_of[13], (D, FF), FF ** -0.5, 0.0625, ((0, 16), (1, 2))),
    }


epsilon = 1e-06
decay_temper = 16.0
highest = lax.Precision.HIGHEST

def rms_rows(row_block, row_gain):
    values = row_block.astype(jnp.float32)
    inverse = lax.rsqrt(lax.optimization_barrier(jnp.mean(values * values, axis=-1, keepdims=True)) + epsilon)
    return (values * inverse * row_gain).astype(jnp.bfloat16)

def one_direction(queries, keyed, valued, log_decay):
    cumulative = jnp.cumsum(log_decay, axis=2)
    block_end = cumulative[:, :, -1:, :]
    q_decayed = queries * jnp.exp(cumulative)
    k_decayed = keyed * jnp.exp(-cumulative)
    block_len = queries.shape[2]
    lower_mask = jnp.tril(jnp.ones((block_len, block_len), dtype=bool))
    scores = jnp.where(lower_mask, jnp.einsum('nhtd,nhsd->nhts', q_decayed, k_decayed, precision=highest), 0.0)
    within = jnp.einsum('nhts,nhsv->nhtv', scores, valued, precision=highest)
    k_tail = keyed * jnp.exp(block_end - cumulative)
    contrib = jnp.einsum('nhsd,nhsv->nhdv', k_tail, valued, precision=highest)
    fading = jnp.exp(block_end[:, :, 0, :])

    def carry_step(state_now, pieces):
        addend, factor = pieces
        return (factor[..., None] * state_now + addend, state_now)
    start_state = jnp.zeros(contrib.shape[1:], jnp.float32)
    _, before = lax.scan(carry_step, start_state, (contrib, fading))
    carried = jnp.einsum('nhtd,nhdv->nhtv', q_decayed, before, precision=highest)
    return within + carried

def mix_heads(queries, keyed, valued, gate_low, gate_up, decay_bias, seq_shift, head_gain):
    length = queries.shape[0]
    head_count = seq_shift.shape[1]
    head_k = queries.shape[1] // head_count
    head_v = valued.shape[1] // head_count
    blocks = length // BLOCK_TOKENS
    gate_pre = jnp.dot(gate_low, gate_up, preferred_element_type=jnp.float32) + decay_bias
    log_decay = jax.nn.log_sigmoid(gate_pre) / decay_temper
    log_decay = log_decay.reshape(length, head_count, head_k) + seq_shift[:, :, None]
    query_f = queries.astype(jnp.float32).reshape(length, head_count, head_k) * head_k ** (-0.5)
    key_f = keyed.astype(jnp.float32).reshape(length, head_count, head_k)
    value_f = valued.astype(jnp.float32).reshape(length, head_count, head_v)

    def to_blocks(tensor):
        return tensor.reshape(blocks, BLOCK_TOKENS, head_count, tensor.shape[-1]).transpose(0, 2, 1, 3)

    def from_blocks(tensor):
        return tensor.transpose(0, 2, 1, 3).reshape(length, head_count, tensor.shape[-1])
    forward = from_blocks(one_direction(to_blocks(query_f), to_blocks(key_f), to_blocks(value_f), to_blocks(log_decay)))
    backward = from_blocks(one_direction(to_blocks(jnp.flip(query_f, 0)), to_blocks(jnp.flip(key_f, 0)), to_blocks(jnp.flip(value_f, 0)), to_blocks(jnp.flip(log_decay, 0))))
    outcome = forward + jnp.flip(backward, 0)
    inverse = lax.rsqrt(lax.optimization_barrier(jnp.mean(outcome * outcome, axis=-1, keepdims=True)) + epsilon)
    normed = outcome * inverse * head_gain.reshape(head_count, head_v)
    return normed.reshape(length, head_count * head_v).astype(jnp.bfloat16)

def group_sum(left, right):
    left_groups = left.astype(jnp.float32).reshape(left.shape[0], N_TP, -1)
    right_groups = right.astype(jnp.float32).reshape(right.shape[0], N_TP, -1)
    terms = jnp.einsum('lgc,dgc->gld', left_groups, right_groups)
    rounded = lax.optimization_barrier(terms.astype(jnp.bfloat16))
    return lax.optimization_barrier(jnp.sum(rounded.astype(jnp.float32), axis=0))

def reference(tokens, mixer_gain, w_query, w_key, w_value, gate_down, gate_up, decay_bias, decay_shift, head_gain, w_out, mlp_gain, mlp_up, mlp_down):
    model_width = tokens.shape[1]

    def one_sequence(pieces):
        seq_rows, seq_shift = pieces
        normed = rms_rows(seq_rows, mixer_gain)
        queries = jnp.dot(normed, w_query, preferred_element_type=jnp.float32).astype(jnp.bfloat16)
        keyed = jnp.dot(normed, w_key, preferred_element_type=jnp.float32).astype(jnp.bfloat16)
        valued = jnp.dot(normed, w_value, preferred_element_type=jnp.float32).astype(jnp.bfloat16)
        gate_low = jnp.dot(normed, gate_down, preferred_element_type=jnp.float32).astype(jnp.bfloat16)
        mixer_out = mix_heads(queries, keyed, valued, gate_low, gate_up, decay_bias, seq_shift, head_gain)
        after_mixer = (seq_rows.astype(jnp.float32) + group_sum(mixer_out, w_out)).astype(jnp.bfloat16)
        normed_two = rms_rows(after_mixer, mlp_gain)
        pre_act = jnp.dot(normed_two, mlp_up, preferred_element_type=jnp.float32)
        hidden = jnp.square(jax.nn.relu(pre_act)).astype(jnp.bfloat16)
        return (after_mixer.astype(jnp.float32) + group_sum(hidden, mlp_down)).astype(jnp.bfloat16)
    sequences = tokens.reshape(-1, SEQUENCE_LENGTH, model_width)
    shifts = decay_shift.reshape(-1, SEQUENCE_LENGTH, decay_shift.shape[1])
    return lax.map(one_sequence, (sequences, shifts)).reshape(tokens.shape)
```

```python
import functools

import jax
import jax.numpy as jnp
from jax import lax
from jax.experimental import pallas as pl
from jax.experimental.pallas import tpu as pltpu
from jax.sharding import Mesh, PartitionSpec as P

BLOCK_TOKENS = 64
SHARE = 4


epsilon = 1e-06
decay_temper = 16.0
highest = lax.Precision.HIGHEST


def rms_rows(row_block, row_gain):
    values = row_block.astype(jnp.float32)
    inverse = lax.rsqrt(jnp.mean(values * values, axis=-1, keepdims=True) + epsilon)
    return (values * inverse * row_gain).astype(jnp.bfloat16)


def mix_heads(
    queries, keyed, valued, gate_low, gate_up, decay_bias, seq_shift, head_gain, sequences
):
    rows = queries.shape[0]
    head_count = seq_shift.shape[1]
    head_k = queries.shape[1] // head_count
    head_v = valued.shape[1] // head_count
    blocks = rows // sequences // BLOCK_TOKENS
    lanes = sequences * head_count
    half = jnp.bfloat16
    full = jnp.float32
    gate_pre = jnp.dot(gate_low, gate_up, preferred_element_type=full) + decay_bias
    log_decay = jax.nn.log_sigmoid(gate_pre) / decay_temper
    log_decay = log_decay.reshape(rows, head_count, head_k) + seq_shift[:, :, None]

    def to_blocks(tensor):
        wide = tensor.reshape(sequences, blocks, BLOCK_TOKENS, head_count, -1)
        wide = wide.transpose(1, 0, 3, 2, 4)
        return wide.reshape(blocks, lanes, BLOCK_TOKENS, -1)

    query_b = to_blocks(queries).astype(full) * head_k ** (-0.5)
    key_b = to_blocks(keyed).astype(full)
    value_b = to_blocks(valued)
    decay_b = to_blocks(log_decay)
    lower = jnp.tril(jnp.ones((BLOCK_TOKENS, BLOCK_TOKENS), full))
    ahead = jnp.einsum("ts,nhsd->nhtd", lower, decay_b, precision=highest)
    back = jnp.einsum("st,nhsd->nhtd", lower, decay_b, precision=highest)
    end = jnp.sum(decay_b, axis=2, keepdims=True)
    q_ahead = (query_b * jnp.exp(ahead)).astype(half)
    q_back = (query_b * jnp.exp(back)).astype(half)
    k_ahead = (key_b * jnp.exp(-ahead)).astype(half)
    k_back = (key_b * jnp.exp(-back)).astype(half)
    score = "nhtd,nhsd->nhts"
    keep = lower > 0
    scores = jnp.where(
        keep, jnp.einsum(score, q_ahead, k_ahead, preferred_element_type=full), 0.0
    ) + jnp.where(keep.T, jnp.einsum(score, q_back, k_back, preferred_element_type=full), 0.0)
    within = jnp.einsum(
        "nhts,nhsv->nhtv", scores.astype(half), value_b, preferred_element_type=full
    )
    tails = jnp.concatenate(
        [key_b * jnp.exp(end - ahead), key_b * jnp.exp(end - back)], axis=-1
    ).astype(half)
    contrib = jnp.einsum("nhsd,nhsv->nhdv", tails, value_b, preferred_element_type=full)
    fading = jnp.exp(end[:, :, 0, :])[..., None]
    before = [jnp.zeros((lanes, head_k, head_v), full)]
    for block in range(blocks - 1):
        before.append(fading[block] * before[-1] + contrib[block, :, :head_k])
    after = [jnp.zeros((lanes, head_k, head_v), full)]
    for block in range(blocks - 1, 0, -1):
        after.append(fading[block] * after[-1] + contrib[block, :, head_k:])
    states = jnp.concatenate(
        [jnp.stack([s.astype(half) for s in before]),
         jnp.stack([s.astype(half) for s in after[::-1]])], axis=2
    )
    both = jnp.concatenate([q_ahead, q_back], axis=-1)
    outcome = within + jnp.einsum("nhtd,nhdv->nhtv", both, states, preferred_element_type=full)
    inverse = lax.rsqrt(jnp.mean(outcome * outcome, axis=-1, keepdims=True) + epsilon)
    outcome = (outcome * inverse).reshape(blocks, sequences, head_count, BLOCK_TOKENS, head_v)
    normed = outcome * head_gain.reshape(head_count, 1, head_v)
    normed = normed.astype(half).transpose(1, 0, 3, 2, 4)
    return normed.reshape(rows, head_count * head_v)


def times_transposed(left, weight_rows):
    return lax.dot_general(
        left, weight_rows, (((1,), (1,)), ((), ())), preferred_element_type=jnp.float32
    )


half = jnp.bfloat16
full = jnp.float32
MESH = pl.DeviceIdType.MESH
VMEM = pl.BlockSpec(memory_space=pltpu.VMEM)
ROW_TILE = 64
COLUMN_TILE = 256


def flip(place, offset):
    bit = 1
    while bit <= offset:
        if offset & bit:
            place = place + bit - 2 * bit * lax.rem(lax.div(place, bit), 2)
        bit *= 2
    return place


def greet(share):
    place, core = lax.axis_index("share"), lax.axis_index("tp")
    barrier = pltpu.get_barrier_semaphore()
    for offset in range(1, share):
        pl.semaphore_signal(
            barrier, inc=1, device_id={"share": flip(place, offset)}, device_id_type=MESH
        )
    pl.semaphore_signal(barrier, inc=1, device_id={"tp": 1 - core}, device_id_type=MESH)
    pl.semaphore_wait(barrier, share)


def remote(source, target, send, receive, device):
    return pltpu.make_async_remote_copy(
        src_ref=source,
        dst_ref=target,
        send_sem=send,
        recv_sem=receive,
        device_id=device,
        device_id_type=MESH,
    )


def block_of(index, size):
    return pl.ds(pl.multiple_of(index * size, size), size)


def exchange_weights(share, weights, targets, send, receive):
    place = lax.axis_index("share")
    copies = []
    for number, (weight, (target, column)) in enumerate(zip(weights, targets)):
        depth = weight.shape[0]
        size = weight.shape[1] // share
        rows = block_of(place, depth)
        for offset in range(share - 1, 0, -1):
            mate = flip(place, offset)
            copy = remote(
                weight.at[:, block_of(mate, size)],
                target.at[rows, pl.ds(column, size)],
                send.at[number, offset],
                receive.at[number, offset],
                {"share": mate},
            )
            copy.start()
            arrival = remote(
                weight.at[:, block_of(mate, size)],
                target.at[block_of(mate, depth), pl.ds(column, size)],
                send.at[number, offset],
                receive.at[number, offset],
                {"share": mate},
            )
            copies.append((copy, arrival))
        target[rows, pl.ds(column, size)] = weight[:, block_of(place, size)]
    return copies


def finish(copies):
    for copy, arrival in copies:
        copy.wait_send()
        arrival.wait_recv()


def weights_kernel(share, q_ref, k_ref, v_ref, o_ref, out_ref, send, receive):
    greet(share)
    weights = (q_ref, k_ref, v_ref, o_ref)
    targets, column = [], 0
    for weight in weights:
        targets.append((out_ref, column))
        column += weight.shape[1] // share
    finish(exchange_weights(share, weights, targets, send, receive))


class Gather:
    def __init__(self, share, part, target, plane_send, plane_receive, pair_send, pair_receive):
        self.share, self.part, self.target = share, part, target
        self.plane_send, self.plane_receive = plane_send, plane_receive
        self.pair_send, self.pair_receive = pair_send, pair_receive
        self.place, self.core = lax.axis_index("share"), lax.axis_index("tp")

    def rows(self, mate, core):
        return block_of(mate * 2 + core, self.part.shape[0])

    def plane(self, offset, arriving):
        mate = flip(self.place, offset)
        owner = mate if arriving else self.place
        return remote(
            self.part,
            self.target.at[self.rows(owner, self.core)],
            self.plane_send.at[offset],
            self.plane_receive.at[offset],
            {"share": mate},
        )

    def pair(self, offset, arriving):
        mate = flip(self.place, offset)
        source = self.part if offset == 0 else self.target.at[self.rows(mate, self.core)]
        return remote(
            source,
            self.target.at[self.rows(mate, 1 - self.core if arriving else self.core)],
            self.pair_send.at[offset],
            self.pair_receive.at[offset],
            {"tp": 1 - self.core},
        )

    def start(self):
        for offset in range(self.share - 1, 0, -1):
            self.plane(offset, False).start()
        self.pair(0, False).start()

    def finish(self):
        self.target[self.rows(self.place, self.core)] = self.part[...]
        for offset in range(1, self.share):
            self.plane(offset, True).wait_recv()
            self.pair(offset, False).start()
        for offset in range(self.share):
            if offset:
                self.plane(offset, False).wait_send()
            self.pair(offset, False).wait_send()
            self.pair(offset, True).wait_recv()


def tokens_kernel(
    share,
    part_ref,
    shift_ref,
    up_ref,
    down_ref,
    rows_ref,
    shifts_ref,
    up_out,
    down_out,
    send,
    receive,
    plane_send,
    plane_receive,
    pair_send,
    pair_receive,
    shift_send,
    shift_receive,
):
    greet(share)
    place = lax.axis_index("share")
    gather = Gather(
        share, part_ref, rows_ref, plane_send, plane_receive, pair_send, pair_receive
    )
    shifts = []
    for offset in range(1, share):
        mate = flip(place, offset)
        pair = [
            remote(
                shift_ref,
                shifts_ref.at[owner],
                shift_send.at[offset],
                shift_receive.at[offset],
                {"share": mate},
            )
            for owner in (place, mate)
        ]
        pair[0].start()
        shifts.append(pair)
    shifts_ref[place] = shift_ref[...]
    copies = exchange_weights(
        share, (up_ref, down_ref), ((up_out, 0), (down_out, 0)), send, receive
    )
    gather.start()
    finish(shifts)
    gather.finish()
    finish(copies)


def product_scatter(share, left_ref, weight_ref, column, base_ref, after_ref, scratch):
    kept, to_pair, from_pair, to_plane, from_plane, sems = scratch
    place, core = lax.axis_index("share"), lax.axis_index("tp")
    length, width = after_ref.shape
    wide = width // 2
    depth = left_ref.shape[1]
    other = 1 - core

    def pair(offset):
        return remote(
            to_pair.at[offset], from_pair.at[offset], sems.at[0, offset], sems.at[1, offset],
            {"tp": other},
        )

    def plane(offset):
        return remote(
            to_plane.at[offset], from_plane.at[offset], sems.at[2, offset], sems.at[3, offset],
            {"share": flip(place, offset)},
        )

    def multiply(offset):
        rows = block_of(flip(place, offset), length)
        for columns, target in ((other, to_pair), (core, kept)):

            @pl.loop(0, wide // COLUMN_TILE)
            def _(tile):
                start = pl.multiple_of(columns * wide + tile * COLUMN_TILE, COLUMN_TILE)
                product = lax.dot_general(
                    left_ref[rows, :],
                    weight_ref[pl.ds(start, COLUMN_TILE), pl.ds(column, depth)],
                    (((1,), (1,)), ((), ())),
                    preferred_element_type=full,
                )
                target[offset, :, block_of(tile, COLUMN_TILE)] = product.astype(half)

            if columns is other:
                pair(offset).start()

    def combine(offset):
        pair(offset).wait_recv()

        @pl.loop(0, length // ROW_TILE)
        def _(tile):
            rows = block_of(tile, ROW_TILE)
            total = kept[offset, rows, :].astype(full) + from_pair[offset, rows, :].astype(full)
            to_plane[offset, rows, :] = total.astype(half)

        if offset:
            plane(offset).start()

    order = list(range(share - 1, -1, -1))
    multiply(order[0])
    for number, offset in enumerate(order):
        if number + 1 < share:
            multiply(order[number + 1])
        combine(offset)
    for offset in order[:-1]:
        plane(offset).wait_recv()
    mine = block_of(core, wide)

    @pl.loop(0, length // ROW_TILE)
    def _(tile):
        rows = block_of(tile, ROW_TILE)
        total = base_ref[rows, mine].astype(full) + to_plane[0, rows, :].astype(full)
        for offset in range(1, share):
            total += from_plane[offset, rows, :].astype(full)
        after_ref[rows, mine] = total.astype(half)

    def swap(arriving):
        columns = block_of(other if arriving else core, wide)
        return remote(
            after_ref.at[:, columns], after_ref.at[:, columns], sems.at[0, share],
            sems.at[1, share], {"tp": other},
        )

    swap(False).start()
    for offset in range(share):
        pair(offset).wait_send()
        if offset:
            plane(offset).wait_send()
    swap(False).wait_send()
    swap(True).wait_recv()


def middle_kernel(
    share,
    column,
    left_ref,
    weight_ref,
    base_ref,
    gain_ref,
    after_ref,
    rows_ref,
    kept,
    to_pair,
    from_pair,
    to_plane,
    from_plane,
    sems,
    part,
    plane_send,
    plane_receive,
    pair_send,
    pair_receive,
):
    greet(share)
    scratch = (kept, to_pair, from_pair, to_plane, from_plane, sems)
    product_scatter(share, left_ref, weight_ref, column, base_ref, after_ref, scratch)
    core = lax.axis_index("tp")
    size = part.shape[0]

    @pl.loop(0, size // 32)
    def _(tile):
        start = pl.multiple_of(core * size + tile * 32, 32)
        values = after_ref[pl.ds(start, 32), :].astype(full)
        inverse = lax.rsqrt(jnp.mean(values * values, axis=-1, keepdims=True) + epsilon)
        part[block_of(tile, 32), :] = (values * inverse * gain_ref[...]).astype(half)

    gather = Gather(share, part, rows_ref, plane_send, plane_receive, pair_send, pair_receive)
    gather.start()
    gather.finish()


def last_kernel(
    share,
    left_ref,
    weight_ref,
    base_ref,
    after_ref,
    kept,
    to_pair,
    from_pair,
    to_plane,
    from_plane,
    sems,
):
    greet(share)
    scratch = (kept, to_pair, from_pair, to_plane, from_plane, sems)
    product_scatter(share, left_ref, weight_ref, 0, base_ref, after_ref, scratch)


def call(kernel, identity, outs, scratch, microseconds, *operands):
    return pl.pallas_call(
        kernel,
        out_shape=outs,
        in_specs=[VMEM] * len(operands),
        out_specs=jax.tree.map(lambda _: VMEM, outs),
        scratch_shapes=scratch,
        compiler_params=pltpu.CompilerParams(collective_id=identity, has_side_effects=True),
        cost_estimate=pl.CostEstimate(
            flops=0, bytes_accessed=microseconds * 3_000_000, transcendentals=0
        ),
    )(*operands)


def scatter_scratch(share, length, width):
    slots = pltpu.VMEM((share, length, width // 2), half)
    return [slots] * 5 + [pltpu.SemaphoreType.DMA((4, share + 1))]


def gather_scratch(share):
    return [pltpu.SemaphoreType.DMA((share,))] * 4


def per_device_shared(
    share,
    tokens,
    mixer_gain,
    w_query,
    w_key,
    w_value,
    gate_down,
    gate_up,
    decay_bias,
    decay_shift,
    head_gain,
    w_out,
    mlp_gain,
    mlp_up,
    mlp_down,
):
    depth = w_query.shape[0]
    length, width = tokens.shape
    place = lax.axis_index("share")
    core = lax.axis_index("tp")
    part = length // 2

    def own_part(array, axis):
        size = array.shape[axis] // share
        return lax.dynamic_slice_in_dim(array, place * size, size, axis)

    def spread(own):
        return lax.all_gather(own, "band", axis=0, tiled=True)

    wide_k = w_query.shape[1] // share
    wide_v = w_value.shape[1] // share
    wide = 2 * wide_k + wide_v
    pairs = [pltpu.SemaphoreType.DMA((4, share))] * 2
    own = call(
        functools.partial(weights_kernel, share),
        0,
        jax.ShapeDtypeStruct((share * depth, wide + wide_v), half),
        pairs,
        12,
        w_query,
        w_key,
        w_value,
        w_out,
    )
    joined = spread(own)
    mine = lax.dynamic_slice_in_dim(tokens, core * part, part, 0)
    heads = decay_shift.shape[1]
    shift_t = jnp.pad(decay_shift.T, ((0, -heads % 8), (0, 0)))
    hidden_wide = mlp_up.shape[1] // share
    weight_out = jax.ShapeDtypeStruct((share * depth, hidden_wide), half)
    rows_shape = jax.ShapeDtypeStruct((share * length, width), half)
    rows_all, shifts, up_own, down_own = call(
        functools.partial(tokens_kernel, share),
        1,
        (
            rows_shape,
            jax.ShapeDtypeStruct((share,) + shift_t.shape, full),
            weight_out,
            weight_out,
        ),
        [pltpu.SemaphoreType.DMA((2, share))] * 2
        + gather_scratch(share)
        + [pltpu.SemaphoreType.DMA((share,))] * 2,
        65,
        rms_rows(mine, mixer_gain),
        shift_t,
        mlp_up,
        mlp_down,
    )
    up_all = spread(up_own)
    down_all = spread(down_own)
    count = heads // share
    shift = lax.dynamic_slice_in_dim(shifts, place * count, count, 1)
    shift = shift.transpose(0, 2, 1).reshape(share * length, count)
    gate_low = jnp.dot(rows_all, gate_down, preferred_element_type=full).astype(half)
    sums = jnp.dot(rows_all, joined[:, :wide], preferred_element_type=full).astype(half)
    query_sum, key_sum, value_sum = jnp.split(sums, (wide_k, 2 * wide_k), axis=1)
    mixer_out = mix_heads(
        query_sum,
        key_sum,
        value_sum,
        gate_low,
        own_part(gate_up, 1),
        own_part(decay_bias, 0),
        shift,
        own_part(head_gain, 0),
        share,
    )
    after_shape = jax.ShapeDtypeStruct((length, width), half)
    after_mixer, rows_two = call(
        functools.partial(middle_kernel, share, wide),
        2,
        (after_shape, rows_shape),
        scatter_scratch(share, length, width)
        + [pltpu.VMEM((part, width), half)]
        + gather_scratch(share),
        95,
        mixer_out,
        joined,
        tokens,
        mlp_gain.reshape(1, width),
    )
    pre = jnp.dot(rows_two, up_all, preferred_element_type=full)
    hidden = jnp.square(jax.nn.relu(pre)).astype(half)
    return call(
        functools.partial(last_kernel, share),
        3,
        after_shape,
        scatter_scratch(share, length, width),
        55,
        hidden,
        down_all,
        after_mixer,
    )


def per_device(
    tokens,
    mixer_gain,
    w_query,
    w_key,
    w_value,
    gate_down,
    gate_up,
    decay_bias,
    decay_shift,
    head_gain,
    w_out,
    mlp_gain,
    mlp_up,
    mlp_down,
):
    rows_all = rms_rows(tokens, mixer_gain)
    gate_low = jnp.dot(rows_all, gate_down, preferred_element_type=jnp.float32).astype(jnp.bfloat16)
    joined = jnp.concatenate([w_query, w_key, w_value], axis=1)
    joined = lax.all_gather(joined, "fs", axis=0, tiled=True)
    sums = jnp.dot(rows_all, joined, preferred_element_type=jnp.float32).astype(jnp.bfloat16)
    wide = w_query.shape[1]
    query_sum, key_sum, value_sum = jnp.split(sums, (wide, 2 * wide), axis=1)
    mixer_out = mix_heads(
        query_sum,
        key_sum,
        value_sum,
        gate_low,
        gate_up,
        decay_bias,
        decay_shift,
        head_gain,
        1,
    )
    out_all = lax.all_gather(w_out, "fs", axis=0, tiled=True)
    mixer_term = times_transposed(mixer_out, out_all).astype(jnp.bfloat16).astype(jnp.float32)
    mixer_sum = lax.psum(mixer_term.astype(jnp.bfloat16), "tp").astype(jnp.float32)
    after_mixer = (tokens.astype(jnp.float32) + mixer_sum).astype(jnp.bfloat16)
    rows_two = rms_rows(after_mixer, mlp_gain)
    up_all, down_all = (
        lax.all_gather(mlp_up, "fs", axis=0, tiled=True),
        lax.all_gather(mlp_down, "fs", axis=0, tiled=True),
    )
    hidden = jnp.square(
        jax.nn.relu(jnp.dot(rows_two, up_all, preferred_element_type=jnp.float32))
    ).astype(jnp.bfloat16)
    mlp_term = times_transposed(hidden, down_all).astype(jnp.bfloat16).astype(jnp.float32)
    mlp_total = lax.psum(mlp_term.astype(jnp.bfloat16), "tp").astype(jnp.float32)
    return (after_mixer.astype(jnp.float32) + mlp_total).astype(jnp.bfloat16)


def solution(mesh):
    bands, cores = mesh.devices.shape
    fs = ("band", "share")
    split = Mesh(mesh.devices.reshape(bands // SHARE, SHARE, cores), fs + ("tp",))

    def layer(*arrays):
        heads = arrays[8].shape[1] // cores
        shared = cores == 2 and heads % SHARE == 0
        axis = fs if shared else "fs"
        body = functools.partial(per_device_shared, SHARE) if shared else per_device
        row, both = P(axis, None), P(axis, "tp")
        return jax.shard_map(
            body,
            mesh=split if shared else mesh,
            in_specs=(
                row, P(), both, both, both, P(), P(None, "tp"), P("tp"), both, P("tp"),
                both, P(), both, both,
            ),
            out_specs=row,
            check_vma=False,
        )(*arrays)

    return layer
```

```python
import functools

import jax
import jax.numpy as jnp
from jax import lax
from jax.experimental import pallas as pl
from jax.experimental.pallas import tpu as pltpu
from jax.sharding import Mesh, PartitionSpec as P

BLOCK_TOKENS = 64
SHARE = 4


epsilon = 1e-06
decay_temper = 16.0
highest = lax.Precision.HIGHEST


def rms_rows(row_block, row_gain):
    values = row_block.astype(jnp.float32)
    inverse = lax.rsqrt(jnp.mean(values * values, axis=-1, keepdims=True) + epsilon)
    return (values * inverse * row_gain).astype(jnp.bfloat16)


def mix_heads(
    queries, keyed, valued, gate_low, gate_up, decay_bias, seq_shift, head_gain, sequences
):
    rows = queries.shape[0]
    head_count = seq_shift.shape[1]
    head_k = queries.shape[1] // head_count
    head_v = valued.shape[1] // head_count
    blocks = rows // sequences // BLOCK_TOKENS
    lanes = sequences * head_count
    half = jnp.bfloat16
    full = jnp.float32
    gate_pre = jnp.dot(gate_low, gate_up, preferred_element_type=full) + decay_bias
    log_decay = jax.nn.log_sigmoid(gate_pre) / decay_temper
    log_decay = log_decay.reshape(rows, head_count, head_k) + seq_shift[:, :, None]

    def to_blocks(tensor):
        wide = tensor.reshape(sequences, blocks, BLOCK_TOKENS, head_count, -1)
        wide = wide.transpose(1, 0, 3, 2, 4)
        return wide.reshape(blocks, lanes, BLOCK_TOKENS, -1)

    query_b = to_blocks(queries).astype(full) * head_k ** (-0.5)
    key_b = to_blocks(keyed).astype(full)
    value_b = to_blocks(valued)
    decay_b = to_blocks(log_decay)
    lower = jnp.tril(jnp.ones((BLOCK_TOKENS, BLOCK_TOKENS), full))
    ahead = jnp.einsum("ts,nhsd->nhtd", lower, decay_b, precision=highest)
    back = jnp.einsum("st,nhsd->nhtd", lower, decay_b, precision=highest)
    end = jnp.sum(decay_b, axis=2, keepdims=True)
    q_ahead = (query_b * jnp.exp(ahead)).astype(half)
    q_back = (query_b * jnp.exp(back)).astype(half)
    k_ahead = (key_b * jnp.exp(-ahead)).astype(half)
    k_back = (key_b * jnp.exp(-back)).astype(half)
    score = "nhtd,nhsd->nhts"
    keep = lower > 0
    scores = jnp.where(
        keep, jnp.einsum(score, q_ahead, k_ahead, preferred_element_type=full), 0.0
    ) + jnp.where(keep.T, jnp.einsum(score, q_back, k_back, preferred_element_type=full), 0.0)
    within = jnp.einsum(
        "nhts,nhsv->nhtv", scores.astype(half), value_b, preferred_element_type=full
    )
    tails = jnp.concatenate(
        [key_b * jnp.exp(end - ahead), key_b * jnp.exp(end - back)], axis=-1
    ).astype(half)
    contrib = jnp.einsum("nhsd,nhsv->nhdv", tails, value_b, preferred_element_type=full)
    fading = jnp.exp(end[:, :, 0, :])[..., None]
    before = [jnp.zeros((lanes, head_k, head_v), full)]
    for block in range(blocks - 1):
        before.append(fading[block] * before[-1] + contrib[block, :, :head_k])
    after = [jnp.zeros((lanes, head_k, head_v), full)]
    for block in range(blocks - 1, 0, -1):
        after.append(fading[block] * after[-1] + contrib[block, :, head_k:])
    states = jnp.concatenate(
        [jnp.stack([s.astype(half) for s in before]),
         jnp.stack([s.astype(half) for s in after[::-1]])], axis=2
    )
    both = jnp.concatenate([q_ahead, q_back], axis=-1)
    outcome = within + jnp.einsum("nhtd,nhdv->nhtv", both, states, preferred_element_type=full)
    inverse = lax.rsqrt(jnp.mean(outcome * outcome, axis=-1, keepdims=True) + epsilon)
    outcome = (outcome * inverse).reshape(blocks, sequences, head_count, BLOCK_TOKENS, head_v)
    normed = outcome * head_gain.reshape(head_count, 1, head_v)
    normed = normed.astype(half).transpose(1, 0, 3, 2, 4)
    return normed.reshape(rows, head_count * head_v)


def times_transposed(left, weight_rows):
    return lax.dot_general(
        left, weight_rows, (((1,), (1,)), ((), ())), preferred_element_type=jnp.float32
    )


half = jnp.bfloat16
full = jnp.float32
MESH = pl.DeviceIdType.MESH
VMEM = pl.BlockSpec(memory_space=pltpu.VMEM)
ROW_TILE = 64
COLUMN_TILE = 256


def flip(place, offset):
    bit = 1
    while bit <= offset:
        if offset & bit:
            place = place + bit - 2 * bit * lax.rem(lax.div(place, bit), 2)
        bit *= 2
    return place


def greet(share, along=False):
    place, core = lax.axis_index("share"), lax.axis_index("tp")
    barrier = pltpu.get_barrier_semaphore()
    if along:
        band, bands = lax.axis_index("band"), lax.axis_size("band")
        for edge, step in ((0, -1), (bands - 1, 1)):

            @pl.when(band != edge)
            def _():
                pl.semaphore_signal(
                    barrier, inc=1, device_id={"band": band + step}, device_id_type=MESH
                )
    for offset in range(1, share):
        pl.semaphore_signal(
            barrier, inc=1, device_id={"share": flip(place, offset)}, device_id_type=MESH
        )
    pl.semaphore_signal(barrier, inc=1, device_id={"tp": 1 - core}, device_id_type=MESH)
    count = share
    if along:
        count = count + jnp.minimum(band, 1) + jnp.minimum(bands - 1 - band, 1)
    pl.semaphore_wait(barrier, count)


def remote(source, target, send, receive, device):
    return pltpu.make_async_remote_copy(
        src_ref=source,
        dst_ref=target,
        send_sem=send,
        recv_sem=receive,
        device_id=device,
        device_id_type=MESH,
    )


def block_of(index, size):
    return pl.ds(pl.multiple_of(index * size, size), size)


def exchange_weights(share, weights, targets, send, receive):
    place = lax.axis_index("share")
    copies = []
    for number, (weight, (target, first, column)) in enumerate(zip(weights, targets)):
        depth = weight.shape[0]
        size = weight.shape[1] // share

        def landing(owner):
            start = pl.multiple_of(first + owner * depth, depth)
            return target.at[pl.ds(start, depth), pl.ds(column, size)]

        for offset in range(share - 1, 0, -1):
            mate = flip(place, offset)
            copy, arrival = [
                remote(
                    weight.at[:, block_of(mate, size)],
                    landing(owner),
                    send.at[number, offset],
                    receive.at[number, offset],
                    {"share": mate},
                )
                for owner in (place, mate)
            ]
            copy.start()
            copies.append((copy, arrival))
        landing(place)[...] = weight[:, block_of(place, size)]
    return copies


def finish(copies):
    for copy, arrival in copies:
        copy.wait_send()
        arrival.wait_recv()


class Chain:
    def __init__(self, target, send, receive):
        self.target, self.send, self.receive = target, send, receive
        self.band, self.bands = lax.axis_index("band"), lax.axis_size("band")
        self.size = target.shape[0] // self.bands

    def copy(self, way, step, block):
        place = self.target.at[block_of(block, self.size)]
        return remote(
            place,
            place,
            self.send.at[way, step],
            self.receive.at[way, step],
            {"band": jnp.clip(self.band + 1 - 2 * way, 0, self.bands - 1)},
        )

    def each(self, step, arriving, action):
        band, bands = self.band, self.bands
        back = step + 1 if arriving else step
        forth = 0 if arriving else 1
        pl.when((band >= back) & (band + forth < bands))(
            lambda: action(self.copy(0, step, band - back))
        )
        pl.when((band + back < bands) & (band >= forth))(
            lambda: action(self.copy(1, step, band + back))
        )

    def start(self, step):
        self.each(step, False, lambda copy: copy.start())

    def arrive(self, step):
        self.each(step, True, lambda copy: copy.wait_recv())

    def finish(self):
        for step in range(self.bands - 1):
            self.each(step, False, lambda copy: copy.wait_send())


X, Y, DIAGONAL = 1, 2, 3
HOPS = ((X, 0), (X, 1), (Y, 0), (Y, 1), (X, 0), (Y, 1))


class Gather:
    def __init__(self, part, target, sems):
        self.part, self.target, self.sems = part, target, sems
        self.place, self.core = lax.axis_index("share"), lax.axis_index("tp")
        self.size = part.shape[0]

    def rows(self, offset, core, piece=None):
        first = (flip(self.place, offset) * 2 + core) * self.size
        size = self.size
        if piece is not None:
            size = self.size // 2
            first = first + piece * size
        return pl.ds(pl.multiple_of(first, size), size)

    def owner(self, slot, arriving):
        way = HOPS[slot][0]
        if slot < 4:
            return way if arriving else 0
        return DIAGONAL if arriving else X + Y - way

    def plane(self, slot, arriving=False):
        way, piece = HOPS[slot]
        rows = self.target.at[self.rows(self.owner(slot, arriving), self.core, piece)]
        source = rows
        if slot < 4:
            half_size = self.size // 2
            source = self.part.at[pl.ds(piece * half_size, half_size)]
        return remote(
            source, rows, self.sems.at[0, slot], self.sems.at[1, slot],
            {"share": flip(self.place, way)},
        )

    def pair(self, slot, arriving=False):
        core = 1 - self.core if arriving else self.core
        if slot == 6:
            source, rows = self.part, self.target.at[self.rows(0, core)]
        else:
            offset = self.owner(slot, True)
            rows = self.target.at[self.rows(offset, core, HOPS[slot][1])]
            source = self.target.at[self.rows(offset, self.core, HOPS[slot][1])]
        return remote(
            source, rows, self.sems.at[2, slot], self.sems.at[3, slot], {"tp": 1 - self.core}
        )

    def start(self):
        for slot in (2, 1, 0, 3):
            self.plane(slot).start()
        self.pair(6).start()
        self.target[self.rows(0, self.core)] = self.part[...]

    def arrive(self, *slots):
        for slot in slots:
            self.plane(slot, True).wait_recv()
            if slot == 2:
                self.plane(4).start()
            if slot == 1:
                self.plane(5).start()
            self.pair(slot).start()

    def from_pair(self, *slots):
        for slot in slots:
            self.pair(slot, True).wait_recv()

    def finish(self):
        for slot in range(7):
            if slot < 6:
                self.plane(slot).wait_send()
            self.pair(slot).wait_send()


def first_kernel(
    share,
    part_ref,
    shift_ref,
    q_ref,
    k_ref,
    v_ref,
    o_ref,
    up_ref,
    down_ref,
    rows_ref,
    shifts_ref,
    joined_ref,
    up_out,
    down_out,
    send,
    receive,
    chain_send,
    chain_receive,
    gather_sems,
    shift_send,
    shift_receive,
):
    chain = Chain(joined_ref, chain_send, chain_receive)
    greet(share, True)
    place = lax.axis_index("share")
    weights = (q_ref, k_ref, v_ref, o_ref)
    targets, column = [], 0
    for weight in weights:
        targets.append((joined_ref, chain.band * chain.size, column))
        column += weight.shape[1] // share
    early = exchange_weights(share, weights, targets, send, receive)
    gather = Gather(part_ref, rows_ref, gather_sems)
    gather.start()
    shifts = []
    for offset in range(1, share):
        mate = flip(place, offset)
        copies = [
            remote(
                shift_ref,
                shifts_ref.at[owner],
                shift_send.at[offset],
                shift_receive.at[offset],
                {"share": mate},
            )
            for owner in (place, mate)
        ]
        copies[0].start()
        shifts.append(copies)
    shifts_ref[place] = shift_ref[...]
    late = exchange_weights(
        share,
        (up_ref, down_ref),
        ((up_out, 0, 0), (down_out, 0, 0)),
        send.at[pl.ds(4, 2)],
        receive.at[pl.ds(4, 2)],
    )
    finish(early)
    chain.start(0)
    gather.arrive(2, 1)
    last = chain.bands - 2
    for step in range(last):
        chain.arrive(step)
        chain.start(step + 1)
        if step == 0:
            gather.arrive(0, 3)
    gather.arrive(4, 5)
    finish(shifts)
    gather.from_pair(*range(7))
    gather.finish()
    chain.arrive(last)
    chain.finish()
    finish(late)


def product_scatter(share, left_ref, weight_ref, column, columns_of, base_ref, scratch, store):
    kept, to_pair, from_pair, to_plane, from_plane, sems = scratch
    place, core = lax.axis_index("share"), lax.axis_index("tp")
    length, wide = kept.shape[1:]
    narrow = wide // 2
    depth = left_ref.shape[1]
    other = 1 - core

    def pair(offset):
        return remote(
            to_pair.at[offset], from_pair.at[offset], sems.at[0, offset], sems.at[1, offset],
            {"tp": other},
        )

    routes = ((3, 0, X), (3, 1, Y), (X, 0, X), (Y, 1, Y), (X, 1, X), (Y, 0, Y))

    def plane(slot):
        offset, piece, way = routes[slot]
        return remote(
            to_plane.at[offset, piece], from_plane.at[slot], sems.at[2, slot],
            sems.at[3, slot], {"share": flip(place, way)},
        )

    def multiply(offset):
        rows = block_of(flip(place, offset), length)
        for side, target in ((other, to_pair), (core, kept)):

            @pl.loop(0, wide // COLUMN_TILE)
            def _(tile):
                start = pl.multiple_of(side * wide + tile * COLUMN_TILE, COLUMN_TILE)
                product = lax.dot_general(
                    left_ref[rows, :],
                    weight_ref[pl.ds(start, COLUMN_TILE), pl.ds(column, depth)],
                    (((1,), (1,)), ((), ())),
                    preferred_element_type=full,
                )
                target[offset, :, block_of(tile, COLUMN_TILE)] = product.astype(half)

            if side is other:
                pair(offset).start()

    def combine(offset):
        pair(offset).wait_recv()

        @pl.loop(0, length // ROW_TILE)
        def _(tile):
            rows = block_of(tile, ROW_TILE)
            total = kept[offset, rows, :].astype(full) + from_pair[offset, rows, :].astype(full)
            total = total.astype(half)
            to_plane[offset, 0, rows, :] = total[:, :narrow]
            to_plane[offset, 1, rows, :] = total[:, narrow:]

    def add(slot, arrived):
        offset, piece, _ = routes[slot]
        plane(arrived).wait_recv()

        @pl.loop(0, length // ROW_TILE)
        def _(tile):
            rows = block_of(tile, ROW_TILE)
            total = to_plane[offset, piece, rows, :].astype(full)
            total += from_plane[arrived, rows, :].astype(full)
            to_plane[offset, piece, rows, :] = total.astype(half)

        plane(slot).start()

    multiply(DIAGONAL)
    multiply(X)
    combine(DIAGONAL)
    plane(0).start()
    plane(1).start()
    multiply(Y)
    combine(X)
    plane(2).start()
    multiply(0)
    combine(Y)
    plane(3).start()
    combine(0)
    add(4, 1)
    add(5, 0)
    for slot in (2, 3, 4, 5):
        plane(slot).wait_recv()

    @pl.loop(0, length // ROW_TILE)
    def _(tile):
        rows = block_of(tile, ROW_TILE)
        for piece, slots in ((0, (2, 5)), (1, (3, 4))):
            total = to_plane[0, piece, rows, :].astype(full)
            for slot in slots:
                total += from_plane[slot, rows, :].astype(full)
            for tile in range(narrow // COLUMN_TILE):
                columns = columns_of(core, piece * (narrow // COLUMN_TILE) + tile)
                value = total[:, tile * COLUMN_TILE : (tile + 1) * COLUMN_TILE]
                value += base_ref[rows, columns].astype(full)
                store(rows, core, piece * narrow + tile * COLUMN_TILE, value.astype(half))

    for offset in range(share):
        pair(offset).wait_send()
    for slot in range(6):
        plane(slot).wait_send()


def swap_halves(ref, sems):
    core = lax.axis_index("tp")
    wide = ref.shape[1] // 2
    copy, arrival = [
        remote(
            ref.at[:, block_of(side, wide)],
            ref.at[:, block_of(side, wide)],
            sems.at[0, 6],
            sems.at[1, 6],
            {"tp": 1 - core},
        )
        for side in (core, 1 - core)
    ]
    copy.start()
    copy.wait_send()
    arrival.wait_recv()


def scatter_kernel(
    share,
    column,
    step,
    shift,
    left_ref,
    weight_ref,
    base_ref,
    out_ref,
    kept,
    to_pair,
    from_pair,
    to_plane,
    from_plane,
    sems,
):
    greet(share)
    wide = out_ref.shape[1] // 2

    def columns_of(core, tile):
        index = (core * (wide // COLUMN_TILE) + tile) * step + shift
        return block_of(index, COLUMN_TILE)

    def store(rows, core, start, value):
        first = pl.multiple_of(core * wide + start, COLUMN_TILE)
        out_ref[rows, pl.ds(first, COLUMN_TILE)] = value

    scratch = (kept, to_pair, from_pair, to_plane, from_plane, sems)
    product_scatter(share, left_ref, weight_ref, column, columns_of, base_ref, scratch, store)
    swap_halves(out_ref, sems)


def hidden_kernel(share, after_ref, gain_ref, up_ref, hidden_ref, rows_ref, part, sems):
    greet(share)
    core = lax.axis_index("tp")
    size = part.shape[0]

    @pl.loop(0, size // 32)
    def _(tile):
        start = pl.multiple_of(core * size + tile * 32, 32)
        values = after_ref[pl.ds(start, 32), :].astype(full)
        inverse = lax.rsqrt(jnp.mean(values * values, axis=-1, keepdims=True) + epsilon)
        part[block_of(tile, 32), :] = (values * inverse * gain_ref[...]).astype(half)

    gather = Gather(part, rows_ref, sems)
    gather.start()

    def product(offset, side):
        rows = gather.rows(offset, side)

        @pl.loop(0, hidden_ref.shape[1] // COLUMN_TILE)
        def _(tile):
            columns = block_of(tile, COLUMN_TILE)
            pre = jnp.dot(rows_ref[rows, :], up_ref[:, columns], preferred_element_type=full)
            hidden_ref[rows, columns] = jnp.square(jnp.maximum(pre, 0.0)).astype(half)

    product(0, core)
    gather.from_pair(6)
    product(0, 1 - core)
    gather.arrive(2, 1, 0, 3)
    product(X, core)
    gather.from_pair(0, 1)
    product(X, 1 - core)
    gather.arrive(4, 5)
    product(Y, core)
    gather.from_pair(2, 3)
    product(Y, 1 - core)
    product(DIAGONAL, core)
    gather.from_pair(4, 5)
    product(DIAGONAL, 1 - core)
    gather.finish()


def call(kernel, identity, outs, scratch, microseconds, *operands):
    return pl.pallas_call(
        kernel,
        out_shape=outs,
        in_specs=[VMEM] * len(operands),
        out_specs=jax.tree.map(lambda _: VMEM, outs),
        scratch_shapes=scratch,
        compiler_params=pltpu.CompilerParams(collective_id=identity, has_side_effects=True),
        cost_estimate=pl.CostEstimate(
            flops=0, bytes_accessed=microseconds * 3_000_000, transcendentals=0
        ),
    )(*operands)


def scatter_scratch(share, length, width):
    slots = pltpu.VMEM((share, length, width // 2), half)
    quarter = pltpu.VMEM((share, 2, length, width // 4), half)
    landed = pltpu.VMEM((6, length, width // 4), half)
    return [slots] * 3 + [quarter, landed, pltpu.SemaphoreType.DMA((4, 7))]


def per_device_shared(
    share,
    tokens,
    mixer_gain,
    w_query,
    w_key,
    w_value,
    gate_down,
    gate_up,
    decay_bias,
    decay_shift,
    head_gain,
    w_out,
    mlp_gain,
    mlp_up,
    mlp_down,
):
    depth = w_query.shape[0]
    length, width = tokens.shape
    place = lax.axis_index("share")
    core = lax.axis_index("tp")
    bands = lax.axis_size("band")
    part = length // 2

    def own_part(array, axis):
        size = array.shape[axis] // share
        return lax.dynamic_slice_in_dim(array, place * size, size, axis)

    def spread(own):
        return lax.all_gather(own, "band", axis=0, tiled=True)

    wide_k = w_query.shape[1] // share
    wide_v = w_value.shape[1] // share
    wide = 2 * wide_k + wide_v
    mine = lax.dynamic_slice_in_dim(tokens, core * part, part, 0)
    heads = decay_shift.shape[1]
    shift_t = jnp.pad(decay_shift.T, ((0, -heads % 8), (0, 0)))
    hidden_wide = mlp_up.shape[1] // share
    weight_out = jax.ShapeDtypeStruct((share * depth, hidden_wide), half)
    rows_shape = jax.ShapeDtypeStruct((share * length, width), half)
    dma = pltpu.SemaphoreType.DMA
    rows_all, shifts, joined, up_own, down_own = call(
        functools.partial(first_kernel, share),
        0,
        (
            rows_shape,
            jax.ShapeDtypeStruct((share,) + shift_t.shape, full),
            jax.ShapeDtypeStruct((width, wide + wide_v), half),
            weight_out,
            weight_out,
        ),
        [dma((6, share))] * 2 + [dma((2, bands))] * 2 + [dma((4, 7))] + [dma((share,))] * 2,
        65,
        rms_rows(mine, mixer_gain),
        shift_t,
        w_query,
        w_key,
        w_value,
        w_out,
        mlp_up,
        mlp_down,
    )
    up_all = spread(up_own)
    split = share * depth // 2
    down_halves = [spread(down_own[:split]), spread(down_own[split:])]
    count = heads // share
    shift = lax.dynamic_slice_in_dim(shifts, place * count, count, 1)
    shift = shift.transpose(0, 2, 1).reshape(share * length, count)
    gate_low = jnp.dot(rows_all, gate_down, preferred_element_type=full).astype(half)
    sums = jnp.dot(rows_all, joined[:, :wide], preferred_element_type=full).astype(half)
    query_sum, key_sum, value_sum = jnp.split(sums, (wide_k, 2 * wide_k), axis=1)
    mixer_out = mix_heads(
        query_sum,
        key_sum,
        value_sum,
        gate_low,
        own_part(gate_up, 1),
        own_part(decay_bias, 0),
        shift,
        own_part(head_gain, 0),
        share,
    )
    after_mixer = call(
        functools.partial(scatter_kernel, share, wide, 1, 0),
        1,
        jax.ShapeDtypeStruct((length, width), half),
        scatter_scratch(share, length, width),
        45,
        mixer_out,
        joined,
        tokens,
    )
    hidden = call(
        functools.partial(hidden_kernel, share),
        2,
        jax.ShapeDtypeStruct((share * length, hidden_wide), half),
        [
            pltpu.VMEM((share * length, width), half),
            pltpu.VMEM((part, width), half),
            dma((4, 7)),
        ],
        45,
        after_mixer,
        mlp_gain.reshape(1, width),
        up_all,
    )
    results = []
    for number, down in enumerate(down_halves):
        result = call(
            functools.partial(scatter_kernel, share, 0, 2, number),
            3 + number,
            jax.ShapeDtypeStruct((length, width // 2), half),
            scatter_scratch(share, length, width // 2),
            25,
            hidden,
            down,
            after_mixer,
        )
        results.append(result.reshape(length, -1, COLUMN_TILE))
    return jnp.stack(results, axis=2).reshape(length, width)


def per_device(
    tokens,
    mixer_gain,
    w_query,
    w_key,
    w_value,
    gate_down,
    gate_up,
    decay_bias,
    decay_shift,
    head_gain,
    w_out,
    mlp_gain,
    mlp_up,
    mlp_down,
):
    rows_all = rms_rows(tokens, mixer_gain)
    gate_low = jnp.dot(rows_all, gate_down, preferred_element_type=jnp.float32).astype(jnp.bfloat16)
    joined = jnp.concatenate([w_query, w_key, w_value], axis=1)
    joined = lax.all_gather(joined, "fs", axis=0, tiled=True)
    sums = jnp.dot(rows_all, joined, preferred_element_type=jnp.float32).astype(jnp.bfloat16)
    wide = w_query.shape[1]
    query_sum, key_sum, value_sum = jnp.split(sums, (wide, 2 * wide), axis=1)
    mixer_out = mix_heads(
        query_sum,
        key_sum,
        value_sum,
        gate_low,
        gate_up,
        decay_bias,
        decay_shift,
        head_gain,
        1,
    )
    out_all = lax.all_gather(w_out, "fs", axis=0, tiled=True)
    mixer_term = times_transposed(mixer_out, out_all).astype(jnp.bfloat16).astype(jnp.float32)
    mixer_sum = lax.psum(mixer_term.astype(jnp.bfloat16), "tp").astype(jnp.float32)
    after_mixer = (tokens.astype(jnp.float32) + mixer_sum).astype(jnp.bfloat16)
    rows_two = rms_rows(after_mixer, mlp_gain)
    up_all, down_all = (
        lax.all_gather(mlp_up, "fs", axis=0, tiled=True),
        lax.all_gather(mlp_down, "fs", axis=0, tiled=True),
    )
    hidden = jnp.square(
        jax.nn.relu(jnp.dot(rows_two, up_all, preferred_element_type=jnp.float32))
    ).astype(jnp.bfloat16)
    mlp_term = times_transposed(hidden, down_all).astype(jnp.bfloat16).astype(jnp.float32)
    mlp_total = lax.psum(mlp_term.astype(jnp.bfloat16), "tp").astype(jnp.float32)
    return (after_mixer.astype(jnp.float32) + mlp_total).astype(jnp.bfloat16)


def solution(mesh):
    bands, cores = mesh.devices.shape
    fs = ("band", "share")
    split = Mesh(mesh.devices.reshape(bands // SHARE, SHARE, cores), fs + ("tp",))

    def layer(*arrays):
        heads = arrays[8].shape[1] // cores
        block = arrays[2].shape[0] // bands * SHARE
        shared = cores == 2 and heads % SHARE == 0 and block == 2 * COLUMN_TILE
        axis = fs if shared else "fs"
        body = functools.partial(per_device_shared, SHARE) if shared else per_device
        row, both = P(axis, None), P(axis, "tp")
        return jax.shard_map(
            body,
            mesh=split if shared else mesh,
            in_specs=(
                row, P(), both, both, both, P(), P(None, "tp"), P("tp"), both, P("tp"),
                both, P(), both, both,
            ),
            out_specs=row,
            check_vma=False,
        )(*arrays)

    return layer
```

```python
import functools

import jax
import jax.numpy as jnp
from jax import lax
from jax.experimental import pallas as pl
from jax.experimental.pallas import tpu as pltpu
from jax.sharding import Mesh, PartitionSpec as P

BLOCK_TOKENS = 64
SHARE = 4


epsilon = 1e-06
decay_temper = 16.0
highest = lax.Precision.HIGHEST


def rms_rows(row_block, row_gain):
    values = row_block.astype(jnp.float32)
    inverse = lax.rsqrt(jnp.mean(values * values, axis=-1, keepdims=True) + epsilon)
    return (values * inverse * row_gain).astype(jnp.bfloat16)


def mix_heads(
    queries, keyed, valued, gate_low, gate_up, decay_bias, seq_shift, head_gain, sequences
):
    rows = queries.shape[0]
    head_count = seq_shift.shape[1]
    head_k = queries.shape[1] // head_count
    head_v = valued.shape[1] // head_count
    blocks = rows // sequences // BLOCK_TOKENS
    lanes = sequences * head_count
    half = jnp.bfloat16
    full = jnp.float32
    gate_pre = jnp.dot(gate_low, gate_up, preferred_element_type=full) + decay_bias
    log_decay = jax.nn.log_sigmoid(gate_pre) / decay_temper
    log_decay = log_decay.reshape(rows, head_count, head_k) + seq_shift[:, :, None]

    def to_blocks(tensor):
        wide = tensor.reshape(sequences, blocks, BLOCK_TOKENS, head_count, -1)
        wide = wide.transpose(1, 0, 3, 2, 4)
        return wide.reshape(blocks, lanes, BLOCK_TOKENS, -1)

    query_b = to_blocks(queries).astype(full) * head_k ** (-0.5)
    key_b = to_blocks(keyed).astype(full)
    value_b = to_blocks(valued)
    decay_b = to_blocks(log_decay)
    lower = jnp.tril(jnp.ones((BLOCK_TOKENS, BLOCK_TOKENS), full))
    ahead = jnp.einsum("ts,nhsd->nhtd", lower, decay_b, precision=highest)
    back = jnp.einsum("st,nhsd->nhtd", lower, decay_b, precision=highest)
    end = jnp.sum(decay_b, axis=2, keepdims=True)
    q_ahead = (query_b * jnp.exp(ahead)).astype(half)
    q_back = (query_b * jnp.exp(back)).astype(half)
    k_ahead = (key_b * jnp.exp(-ahead)).astype(half)
    k_back = (key_b * jnp.exp(-back)).astype(half)
    score = "nhtd,nhsd->nhts"
    keep = lower > 0
    scores = jnp.where(
        keep, jnp.einsum(score, q_ahead, k_ahead, preferred_element_type=full), 0.0
    ) + jnp.where(keep.T, jnp.einsum(score, q_back, k_back, preferred_element_type=full), 0.0)
    within = jnp.einsum(
        "nhts,nhsv->nhtv", scores.astype(half), value_b, preferred_element_type=full
    )
    tails = jnp.concatenate(
        [key_b * jnp.exp(end - ahead), key_b * jnp.exp(end - back)], axis=-1
    ).astype(half)
    contrib = jnp.einsum("nhsd,nhsv->nhdv", tails, value_b, preferred_element_type=full)
    fading = jnp.exp(end[:, :, 0, :])[..., None]
    before = [jnp.zeros((lanes, head_k, head_v), full)]
    for block in range(blocks - 1):
        before.append(fading[block] * before[-1] + contrib[block, :, :head_k])
    after = [jnp.zeros((lanes, head_k, head_v), full)]
    for block in range(blocks - 1, 0, -1):
        after.append(fading[block] * after[-1] + contrib[block, :, head_k:])
    states = jnp.concatenate(
        [jnp.stack([s.astype(half) for s in before]),
         jnp.stack([s.astype(half) for s in after[::-1]])], axis=2
    )
    both = jnp.concatenate([q_ahead, q_back], axis=-1)
    outcome = within + jnp.einsum("nhtd,nhdv->nhtv", both, states, preferred_element_type=full)
    inverse = lax.rsqrt(jnp.mean(outcome * outcome, axis=-1, keepdims=True) + epsilon)
    outcome = (outcome * inverse).reshape(blocks, sequences, head_count, BLOCK_TOKENS, head_v)
    normed = outcome * head_gain.reshape(head_count, 1, head_v)
    normed = normed.astype(half).transpose(1, 0, 3, 2, 4)
    return normed.reshape(rows, head_count * head_v)


def times_transposed(left, weight_rows):
    return lax.dot_general(
        left, weight_rows, (((1,), (1,)), ((), ())), preferred_element_type=jnp.float32
    )


half = jnp.bfloat16
full = jnp.float32
MESH = pl.DeviceIdType.MESH
VMEM = pl.BlockSpec(memory_space=pltpu.VMEM)
ROW_TILE = 64
COLUMN_TILE = 256


def flip(place, offset):
    bit = 1
    while bit <= offset:
        if offset & bit:
            place = place + bit - 2 * bit * lax.rem(lax.div(place, bit), 2)
        bit *= 2
    return place


def greet(share, along=False):
    place, core = lax.axis_index("share"), lax.axis_index("tp")
    barrier = pltpu.get_barrier_semaphore()
    if along:
        band, bands = lax.axis_index("band"), lax.axis_size("band")
        for edge, step in ((0, -1), (bands - 1, 1)):

            @pl.when(band != edge)
            def _():
                pl.semaphore_signal(
                    barrier, inc=1, device_id={"band": band + step}, device_id_type=MESH
                )
    for offset in range(1, share):
        pl.semaphore_signal(
            barrier, inc=1, device_id={"share": flip(place, offset)}, device_id_type=MESH
        )
    if share:
        pl.semaphore_signal(barrier, inc=1, device_id={"tp": 1 - core}, device_id_type=MESH)
    count = share
    if along:
        count = count + jnp.minimum(band, 1) + jnp.minimum(bands - 1 - band, 1)
    pl.semaphore_wait(barrier, count)


def remote(source, target, send, receive, device):
    return pltpu.make_async_remote_copy(
        src_ref=source,
        dst_ref=target,
        send_sem=send,
        recv_sem=receive,
        device_id=device,
        device_id_type=MESH,
    )


def block_of(index, size):
    return pl.ds(pl.multiple_of(index * size, size), size)


def exchange_weights(share, pieces, send, receive):
    place = lax.axis_index("share")
    copies = []
    for number, (weight, skip, size, target, first, column) in enumerate(pieces):
        depth = weight.shape[0]
        stride = weight.shape[1] // share

        def columns(mate):
            return pl.ds(pl.multiple_of(mate * stride + skip, 128), size)

        def landing(owner):
            start = pl.multiple_of(first + owner * depth, depth)
            return target.at[pl.ds(start, depth), pl.ds(column, size)]

        for offset in range(share - 1, 0, -1):
            mate = flip(place, offset)
            copy, arrival = [
                remote(
                    weight.at[:, columns(mate)],
                    landing(owner),
                    send.at[number, offset],
                    receive.at[number, offset],
                    {"share": mate},
                )
                for owner in (place, mate)
            ]
            copy.start()
            copies.append((copy, arrival))
        landing(place)[...] = weight[:, columns(place)]
    return copies


def finish(copies):
    for copy, arrival in copies:
        copy.wait_send()
        arrival.wait_recv()


class Chain:
    def __init__(self, target, send, receive, own=None):
        self.target, self.send, self.receive, self.own = target, send, receive, own
        self.band, self.bands = lax.axis_index("band"), lax.axis_size("band")
        self.size = target.shape[0] // self.bands

    def copy(self, way, step, block):
        place = self.target.at[block_of(block, self.size)]
        return remote(
            self.own if step == 0 and self.own is not None else place,
            place,
            self.send.at[way, step],
            self.receive.at[way, step],
            {"band": jnp.clip(self.band + 1 - 2 * way, 0, self.bands - 1)},
        )

    def each(self, step, arriving, action):
        band, bands = self.band, self.bands
        back = step + 1 if arriving else step
        forth = 0 if arriving else 1
        pl.when((band >= back) & (band + forth < bands))(
            lambda: action(self.copy(0, step, band - back))
        )
        pl.when((band + back < bands) & (band >= forth))(
            lambda: action(self.copy(1, step, band + back))
        )

    def start(self, step=0):
        self.each(step, False, lambda copy: copy.start())
        if step == 0 and self.own is not None:
            self.target[block_of(self.band, self.size)] = self.own[...]

    def arrive(self, step):
        self.each(step, True, lambda copy: copy.wait_recv())

    def forward(self, step):
        self.arrive(step)
        if step < self.bands - 2:
            self.start(step + 1)

    def finish(self):
        for step in range(self.bands - 1):
            self.each(step, False, lambda copy: copy.wait_send())


X, Y, DIAGONAL = 1, 2, 3
HOPS = ((X, 0), (X, 1), (Y, 0), (Y, 1), (X, 0), (Y, 1))


class Gather:
    def __init__(self, part, target, sems):
        self.part, self.target, self.sems = part, target, sems
        self.place, self.core = lax.axis_index("share"), lax.axis_index("tp")
        self.size = part.shape[0]

    def rows(self, offset, core, piece=None):
        first = (flip(self.place, offset) * 2 + core) * self.size
        size = self.size
        if piece is not None:
            size = self.size // 2
            first = first + piece * size
        return pl.ds(pl.multiple_of(first, size), size)

    def owner(self, slot, arriving):
        way = HOPS[slot][0]
        if slot < 4:
            return way if arriving else 0
        return DIAGONAL if arriving else X + Y - way

    def plane(self, slot, arriving=False):
        way, piece = HOPS[slot]
        rows = self.target.at[self.rows(self.owner(slot, arriving), self.core, piece)]
        source = rows
        if slot < 4:
            half_size = self.size // 2
            source = self.part.at[pl.ds(piece * half_size, half_size)]
        return remote(
            source, rows, self.sems.at[0, slot], self.sems.at[1, slot],
            {"share": flip(self.place, way)},
        )

    def pair(self, slot, arriving=False):
        core = 1 - self.core if arriving else self.core
        if slot == 6:
            source, rows = self.part, self.target.at[self.rows(0, core)]
        else:
            offset = self.owner(slot, True)
            rows = self.target.at[self.rows(offset, core, HOPS[slot][1])]
            source = self.target.at[self.rows(offset, self.core, HOPS[slot][1])]
        return remote(
            source, rows, self.sems.at[2, slot], self.sems.at[3, slot], {"tp": 1 - self.core}
        )

    def start(self):
        for slot in (2, 1, 0, 3):
            self.plane(slot).start()
        self.pair(6).start()
        self.target[self.rows(0, self.core)] = self.part[...]

    def arrive(self, *slots):
        for slot in slots:
            self.plane(slot, True).wait_recv()
            if slot == 2:
                self.plane(4).start()
            if slot == 1:
                self.plane(5).start()
            self.pair(slot).start()

    def from_pair(self, *slots):
        for slot in slots:
            self.pair(slot, True).wait_recv()

    def finish(self):
        for slot in range(7):
            if slot < 6:
                self.plane(slot).wait_send()
            self.pair(slot).wait_send()


def norm_part(source_ref, gain_ref, part):
    core = lax.axis_index("tp")
    size = part.shape[0]

    @pl.loop(0, size // 32)
    def _(tile):
        start = pl.multiple_of(core * size + tile * 32, 32)
        values = source_ref[pl.ds(start, 32), :].astype(full)
        inverse = lax.rsqrt(jnp.mean(values * values, axis=-1, keepdims=True) + epsilon)
        part[block_of(tile, 32), :] = (values * inverse * gain_ref[...]).astype(half)


def first_kernel(
    share,
    tokens_ref,
    gain_ref,
    shift_ref,
    q_ref,
    k_ref,
    v_ref,
    o_ref,
    up_ref,
    down_ref,
    rows_ref,
    shifts_ref,
    joined_ref,
    up_one,
    up_two,
    up_three,
    down_one,
    down_two,
    part,
    send,
    receive,
    chain_sems,
    gather_sems,
    shift_send,
    shift_receive,
):
    chain = Chain(joined_ref, chain_sems.at[0], chain_sems.at[1])
    later = Chain(up_one, chain_sems.at[2], chain_sems.at[3])
    greet(share, True)
    place = lax.axis_index("share")
    base = chain.band * chain.size
    pieces, column = [], 0
    for weight in (q_ref, k_ref, v_ref, o_ref):
        size = weight.shape[1] // share
        pieces.append((weight, 0, size, joined_ref, base, column))
        column += size
    early = exchange_weights(share, pieces, send, receive)
    norm_part(tokens_ref, gain_ref, part)
    gather = Gather(part, rows_ref, gather_sems)
    gather.start()
    shifts = []
    for offset in range(1, share):
        mate = flip(place, offset)
        copies = [
            remote(
                shift_ref,
                shifts_ref.at[owner],
                shift_send.at[offset],
                shift_receive.at[offset],
                {"share": mate},
            )
            for owner in (place, mate)
        ]
        copies[0].start()
        shifts.append(copies)
    shifts_ref[place] = shift_ref[...]
    pieces = []
    for weight, targets in ((up_ref, (up_one, up_two, up_three)), (down_ref, (down_one, down_two))):
        skip = 0
        for target in targets:
            size = target.shape[1]
            pieces.append((weight, skip, size, target, base if target is up_one else 0, 0))
            skip += size
    late = exchange_weights(
        share, pieces, send.at[pl.ds(4, 5)], receive.at[pl.ds(4, 5)]
    )
    finish(early)
    chain.start()
    gather.arrive(2, 1)
    steps = chain.bands - 1
    for step in range(steps - 1):
        chain.forward(step)
        if step == 0:
            gather.arrive(0, 3)
    gather.arrive(4, 5)
    ready = share - 1
    finish(late[:ready])
    later.start()
    finish(shifts)
    gather.from_pair(*range(7))
    gather.finish()
    chain.forward(steps - 1)
    for step in range(steps):
        later.forward(step)
    finish(late[ready:])
    chain.finish()
    later.finish()


def attention_kernel(
    rows_ref,
    joined_ref,
    gate_down_ref,
    gate_up_ref,
    bias_ref,
    shift_ref,
    gain_ref,
    own_ref,
    mixer_ref,
    target_ref,
    total_decay,
    both_ref,
    ahead_ref,
    back_ref,
    tails_ref,
    values_ref,
    added_ref,
    states_ref,
    result_ref,
    chain_sems,
):
    chain = Chain(target_ref, chain_sems.at[0], chain_sems.at[1], own_ref)
    greet(0, True)
    chain.start()
    length = both_ref.shape[0]
    count = rows_ref.shape[0] // length

    @pl.loop(0, count)
    def _(sequence):
        attend(
            block_of(sequence, length), rows_ref, joined_ref, gate_down_ref, gate_up_ref,
            bias_ref, shift_ref, gain_ref, mixer_ref, total_decay, both_ref, ahead_ref,
            back_ref, tails_ref, values_ref, added_ref, states_ref, result_ref,
        )
        for step in range(chain.bands - 1):
            after = min(step + 1, count - 1)

            @pl.when(sequence == after)
            def _():
                chain.forward(step)

    chain.finish()


GROUP = 256


def attend(
    rows,
    rows_ref,
    joined_ref,
    gate_down_ref,
    gate_up_ref,
    bias_ref,
    shift_ref,
    gain_ref,
    mixer_ref,
    total_decay,
    both_ref,
    ahead_ref,
    back_ref,
    tails_ref,
    values_ref,
    added_ref,
    states_ref,
    result_ref,
):
    length, head_k = ahead_ref.shape
    head_v = values_ref.shape[1]
    blocks = length // BLOCK_TOKENS

    def dot(left, right, contract=((1,), (0,)), **options):
        return lax.dot_general(
            left, right, (contract, ((), ())), preferred_element_type=full, **options
        )

    row = lax.broadcasted_iota(jnp.int32, (GROUP, GROUP), 0)
    column = lax.broadcasted_iota(jnp.int32, (GROUP, GROUP), 1)
    same = row // BLOCK_TOKENS == column // BLOCK_TOKENS
    lower = same & (row >= column)
    upper = same & (row <= column)
    lower_f = lower.astype(full)
    upper_f = upper.astype(full)

    for group in range(length // GROUP):
        here = slice(group * GROUP, (group + 1) * GROUP)
        these = pl.ds(pl.multiple_of(rows.start + group * GROUP, GROUP), GROUP)
        row_block = rows_ref[these, :]
        gate_low = dot(row_block, gate_down_ref[...]).astype(half)
        gate_pre = dot(gate_low, gate_up_ref[...]) + bias_ref[...]
        sigmoid = jnp.minimum(gate_pre, 0.0) - jnp.log1p(jnp.exp(-jnp.abs(gate_pre)))
        log_decay = sigmoid / decay_temper + shift_ref[these, :]
        ahead = dot(lower_f, log_decay, precision=highest)
        back = dot(upper_f, log_decay, precision=highest)
        per_block = log_decay.reshape(GROUP // BLOCK_TOKENS, BLOCK_TOKENS, head_k)
        end = jnp.sum(per_block, axis=1, keepdims=True)
        wide_end = jnp.broadcast_to(end, per_block.shape).reshape(GROUP, head_k)
        for block in range(GROUP // BLOCK_TOKENS):
            number = group * (GROUP // BLOCK_TOKENS) + block
            total_decay[number] = jnp.exp(
                jnp.broadcast_to(end[block], (8, head_k))
            )
        queries = dot(row_block, joined_ref[:, :head_k]).astype(half).astype(full)
        queries = queries * head_k ** (-0.5)
        keyed = dot(row_block, joined_ref[:, head_k : 2 * head_k]).astype(half).astype(full)
        values = dot(row_block, joined_ref[:, 2 * head_k : 2 * head_k + head_v]).astype(half)
        q_ahead = (queries * jnp.exp(ahead)).astype(half)
        q_back = (queries * jnp.exp(back)).astype(half)
        k_ahead = (keyed * jnp.exp(-ahead)).astype(half)
        k_back = (keyed * jnp.exp(-back)).astype(half)
        both_ref[here, :head_k] = q_ahead
        both_ref[here, head_k:] = q_back
        tails_ref[here, :head_k] = (keyed * jnp.exp(wide_end - ahead)).astype(half)
        tails_ref[here, head_k:] = (keyed * jnp.exp(wide_end - back)).astype(half)
        values_ref[here, :] = values
        scores = jnp.where(lower, dot(q_ahead, k_ahead, ((1,), (1,))), 0.0)
        scores += jnp.where(upper, dot(q_back, k_back, ((1,), (1,))), 0.0)
        result_ref[here, :] = dot(scores.astype(half), values)
    for block in range(blocks):
        here = slice(block * BLOCK_TOKENS, (block + 1) * BLOCK_TOKENS)
        added_ref[block] = dot(values_ref[here, :], tails_ref[here, :], ((0,), (0,)))
    state = jnp.zeros((head_v, head_k), full)
    for block in range(blocks):
        states_ref[block, :, :head_k] = state.astype(half)
        if block + 1 < blocks:
            state = total_decay[block, :1] * state + added_ref[block, :, :head_k]
    state = jnp.zeros((head_v, head_k), full)
    for block in range(blocks - 1, -1, -1):
        states_ref[block, :, head_k:] = state.astype(half)
        if block:
            state = total_decay[block, :1] * state + added_ref[block, :, head_k:]
    for block in range(blocks):
        here = slice(block * BLOCK_TOKENS, (block + 1) * BLOCK_TOKENS)
        carried = dot(both_ref[here, :], states_ref[block], ((1,), (1,)))
        outcome = result_ref[here, :] + carried
        inverse = lax.rsqrt(jnp.mean(outcome * outcome, axis=-1, keepdims=True) + epsilon)
        these = pl.ds(pl.multiple_of(rows.start + block * BLOCK_TOKENS, BLOCK_TOKENS), BLOCK_TOKENS)
        mixer_ref[these, :] = (outcome * inverse * gain_ref[...]).astype(half)


def product_scatter(share, left_ref, weights, base_ref, out_ref, scratch, between):
    kept, to_pair, from_pair, to_plane, from_plane, sems = scratch
    place, core = lax.axis_index("share"), lax.axis_index("tp")
    length, wide = kept.shape[1:]
    narrow = wide // 2
    other = 1 - core

    def pair(offset):
        return remote(
            to_pair.at[offset], from_pair.at[offset], sems.at[0, offset], sems.at[1, offset],
            {"tp": other},
        )

    routes = ((3, 0, X), (3, 1, Y), (X, 0, X), (Y, 1, Y), (X, 1, X), (Y, 0, Y))

    def plane(slot):
        offset, piece, way = routes[slot]
        return remote(
            to_plane.at[offset, piece], from_plane.at[slot], sems.at[2, slot],
            sems.at[3, slot], {"share": flip(place, way)},
        )

    def multiply(offset):
        rows = block_of(flip(place, offset), length)
        for side, target in ((other, to_pair), (core, kept)):

            @pl.loop(0, wide // COLUMN_TILE)
            def _(tile):
                start = pl.multiple_of(side * wide + tile * COLUMN_TILE, COLUMN_TILE)
                product, first = 0.0, 0
                for weight, column, depth in weights:
                    product += lax.dot_general(
                        left_ref[rows, pl.ds(first, depth)],
                        weight[pl.ds(start, COLUMN_TILE), pl.ds(column, depth)],
                        (((1,), (1,)), ((), ())),
                        preferred_element_type=full,
                    )
                    first += depth
                target[offset, :, block_of(tile, COLUMN_TILE)] = product.astype(half)

            if side is other:
                pair(offset).start()

    def combine(offset):
        pair(offset).wait_recv()

        @pl.loop(0, length // ROW_TILE)
        def _(tile):
            rows = block_of(tile, ROW_TILE)
            total = kept[offset, rows, :].astype(full) + from_pair[offset, rows, :].astype(full)
            total = total.astype(half)
            to_plane[offset, 0, rows, :] = total[:, :narrow]
            to_plane[offset, 1, rows, :] = total[:, narrow:]

    def add(slot, arrived):
        offset, piece, _ = routes[slot]
        plane(arrived).wait_recv()

        @pl.loop(0, length // ROW_TILE)
        def _(tile):
            rows = block_of(tile, ROW_TILE)
            total = to_plane[offset, piece, rows, :].astype(full)
            total += from_plane[arrived, rows, :].astype(full)
            to_plane[offset, piece, rows, :] = total.astype(half)

        plane(slot).start()

    multiply(DIAGONAL)
    multiply(X)
    combine(DIAGONAL)
    plane(0).start()
    plane(1).start()
    multiply(Y)
    combine(X)
    plane(2).start()
    multiply(0)
    combine(Y)
    plane(3).start()
    combine(0)
    add(4, 1)
    add(5, 0)
    between(0)
    plane(2).wait_recv()
    plane(3).wait_recv()
    between(1)
    for slot in (4, 5):
        plane(slot).wait_recv()

    @pl.loop(0, length // ROW_TILE)
    def _(tile):
        rows = block_of(tile, ROW_TILE)
        for piece, slots in ((0, (2, 5)), (1, (3, 4))):
            total = to_plane[0, piece, rows, :].astype(full)
            for slot in slots:
                total += from_plane[slot, rows, :].astype(full)
            columns = pl.ds(pl.multiple_of(core * wide + piece * narrow, narrow), narrow)
            total += base_ref[rows, columns].astype(full)
            out_ref[rows, columns] = total.astype(half)

    swap_halves(out_ref, sems)
    for offset in range(share):
        pair(offset).wait_send()
    for slot in range(6):
        plane(slot).wait_send()


def swap_halves(ref, sems):
    core = lax.axis_index("tp")
    wide = ref.shape[1] // 2
    copy, arrival = [
        remote(
            ref.at[:, block_of(side, wide)],
            ref.at[:, block_of(side, wide)],
            sems.at[0, 6],
            sems.at[1, 6],
            {"tp": 1 - core},
        )
        for side in (core, 1 - core)
    ]
    copy.start()
    copy.wait_send()
    arrival.wait_recv()


def mixer_kernel(
    share,
    column,
    left_ref,
    weight_ref,
    base_ref,
    up_own,
    down_own,
    out_ref,
    up_target,
    down_target,
    kept,
    to_pair,
    from_pair,
    to_plane,
    from_plane,
    sems,
    chain_sems,
):
    greet(share, True)
    chains = (
        Chain(up_target, chain_sems.at[0], chain_sems.at[1], up_own),
        Chain(down_target, chain_sems.at[2], chain_sems.at[3], down_own),
    )
    for chain in chains:
        chain.start()
    steps = chains[0].bands - 1

    def between(step):
        if step < steps:
            for chain in chains:
                chain.forward(step)

    scratch = (kept, to_pair, from_pair, to_plane, from_plane, sems)
    weights = ((weight_ref, column, left_ref.shape[1]),)
    product_scatter(share, left_ref, weights, base_ref, out_ref, scratch, between)
    for step in range(2, steps):
        between(step)
    for chain in chains:
        chain.finish()


def last_kernel(
    share,
    left_ref,
    one_ref,
    two_ref,
    base_ref,
    out_ref,
    kept,
    to_pair,
    from_pair,
    to_plane,
    from_plane,
    sems,
):
    greet(share)
    scratch = (kept, to_pair, from_pair, to_plane, from_plane, sems)
    weights = tuple((ref, 0, ref.shape[1]) for ref in (one_ref, two_ref))
    product_scatter(share, left_ref, weights, base_ref, out_ref, scratch, lambda step: None)


def hidden_kernel(
    share,
    after_ref,
    gain_ref,
    up_one,
    up_two,
    up_three,
    down_own,
    hidden_ref,
    down_target,
    rows_ref,
    part,
    sems,
    chain_sems,
):
    greet(share, True)
    chain = Chain(down_target, chain_sems.at[0], chain_sems.at[1], down_own)
    chain.start()
    core = lax.axis_index("tp")
    norm_part(after_ref, gain_ref, part)
    gather = Gather(part, rows_ref, sems)
    gather.start()

    def product(offset, side):
        rows = gather.rows(offset, side)
        first = 0
        for up_ref in (up_one, up_two, up_three):
            begin = first

            @pl.loop(0, up_ref.shape[1] // COLUMN_TILE)
            def _(tile):
                columns = block_of(tile, COLUMN_TILE)
                pre = jnp.dot(rows_ref[rows, :], up_ref[:, columns], preferred_element_type=full)
                start = pl.multiple_of(begin + tile * COLUMN_TILE, COLUMN_TILE)
                squared = jnp.square(jnp.maximum(pre, 0.0)).astype(half)
                hidden_ref[rows, pl.ds(start, COLUMN_TILE)] = squared

            first += up_ref.shape[1]

    steps = chain.bands - 1
    product(0, core)
    gather.from_pair(6)
    product(0, 1 - core)
    gather.arrive(2, 1)
    chain.forward(0)
    gather.arrive(0, 3)
    product(X, core)
    gather.from_pair(0, 1)
    product(X, 1 - core)
    gather.arrive(4, 5)
    for step in range(1, steps - 1):
        chain.forward(step)
    product(Y, core)
    gather.from_pair(2, 3)
    product(Y, 1 - core)
    product(DIAGONAL, core)
    gather.from_pair(4, 5)
    product(DIAGONAL, 1 - core)
    gather.finish()
    chain.arrive(steps - 1)
    chain.finish()


def call(kernel, identity, outs, scratch, microseconds, *operands):
    return pl.pallas_call(
        kernel,
        out_shape=outs,
        in_specs=[VMEM] * len(operands),
        out_specs=jax.tree.map(lambda _: VMEM, outs),
        scratch_shapes=scratch,
        compiler_params=pltpu.CompilerParams(collective_id=identity, has_side_effects=True),
        cost_estimate=pl.CostEstimate(
            flops=0, bytes_accessed=microseconds * 3_000_000, transcendentals=0
        ),
    )(*operands)


def scatter_scratch(share, length, width):
    slots = pltpu.VMEM((share, length, width // 2), half)
    quarter = pltpu.VMEM((share, 2, length, width // 4), half)
    landed = pltpu.VMEM((6, length, width // 4), half)
    return [slots] * 3 + [quarter, landed, pltpu.SemaphoreType.DMA((4, 7))]


def per_device_shared(
    share,
    tokens,
    mixer_gain,
    w_query,
    w_key,
    w_value,
    gate_down,
    gate_up,
    decay_bias,
    decay_shift,
    head_gain,
    w_out,
    mlp_gain,
    mlp_up,
    mlp_down,
):
    depth = w_query.shape[0]
    length, width = tokens.shape
    place = lax.axis_index("share")
    core = lax.axis_index("tp")
    bands = lax.axis_size("band")
    part = length // 2

    def own_part(array, axis):
        size = array.shape[axis] // share
        return lax.dynamic_slice_in_dim(array, place * size, size, axis)

    def weight(rows, columns):
        return jax.ShapeDtypeStruct((rows, columns), half)

    wide_k = w_query.shape[1] // share
    wide_v = w_value.shape[1] // share
    wide = 2 * wide_k + wide_v
    heads = decay_shift.shape[1]
    shift_t = jnp.pad(decay_shift.T, ((0, -heads % 8), (0, 0)))
    hidden_wide = mlp_up.shape[1] // share
    eighth = hidden_wide // 8
    up_cuts = (2 * eighth, 2 * eighth, 4 * eighth)
    down_cuts = (2 * eighth, 6 * eighth)
    own_rows = share * depth
    rows_shape = weight(share * length, width)
    dma = pltpu.SemaphoreType.DMA
    gain_row = mixer_gain.reshape(1, width)
    rows_all, shifts, joined, up_one, up_two, up_three, down_one, down_two = call(
        functools.partial(first_kernel, share),
        0,
        (
            rows_shape,
            jax.ShapeDtypeStruct((share,) + shift_t.shape, full),
            weight(width, wide + wide_v),
            weight(width, up_cuts[0]),
            weight(own_rows, up_cuts[1]),
            weight(own_rows, up_cuts[2]),
            weight(own_rows, down_cuts[0]),
            weight(own_rows, down_cuts[1]),
        ),
        [pltpu.VMEM((part, width), half)]
        + [dma((9, share))] * 2
        + [dma((4, 2, bands)), dma((4, 7))]
        + [dma((share,))] * 2,
        65,
        tokens,
        gain_row,
        shift_t,
        w_query,
        w_key,
        w_value,
        w_out,
        mlp_up,
        mlp_down,
    )
    shift = lax.dynamic_slice_in_dim(shifts, place, 1, 1)
    shift = shift.reshape(share * length, 1)
    blocks = length // BLOCK_TOKENS
    mixer_out, up_two = call(
        attention_kernel,
        1,
        (weight(share * length, wide_v), weight(width, up_cuts[1])),
        [
            pltpu.VMEM((blocks, 8, wide_k), full),
            pltpu.VMEM((length, 2 * wide_k), half),
            pltpu.VMEM((length, wide_k), half),
            pltpu.VMEM((length, wide_k), half),
            pltpu.VMEM((length, 2 * wide_k), half),
            pltpu.VMEM((length, wide_v), half),
            pltpu.VMEM((blocks, wide_v, 2 * wide_k), full),
            pltpu.VMEM((blocks, wide_v, 2 * wide_k), half),
            pltpu.VMEM((length, wide_v), full),
            dma((2, 2, bands)),
        ],
        25,
        rows_all,
        joined,
        gate_down,
        own_part(gate_up, 1),
        own_part(decay_bias, 0).reshape(1, wide_k),
        shift,
        own_part(head_gain, 0).reshape(1, wide_v),
        up_two,
    )
    after_mixer, up_three, down_one = call(
        functools.partial(mixer_kernel, share, wide),
        2,
        (weight(length, width), weight(width, up_cuts[2]), weight(width, down_cuts[0])),
        scatter_scratch(share, length, width) + [dma((4, 2, bands))],
        45,
        mixer_out,
        joined,
        tokens,
        up_three,
        down_one,
    )
    hidden, down_two = call(
        functools.partial(hidden_kernel, share),
        3,
        (weight(share * length, hidden_wide), weight(width, down_cuts[1])),
        [
            pltpu.VMEM((share * length, width), half),
            pltpu.VMEM((part, width), half),
            dma((4, 7)),
            dma((2, 2, bands)),
        ],
        45,
        after_mixer,
        mlp_gain.reshape(1, width),
        up_one,
        up_two,
        up_three,
        down_two,
    )
    return call(
        functools.partial(last_kernel, share),
        4,
        weight(length, width),
        scatter_scratch(share, length, width),
        45,
        hidden,
        down_one,
        down_two,
        after_mixer,
    )


def per_device(
    tokens,
    mixer_gain,
    w_query,
    w_key,
    w_value,
    gate_down,
    gate_up,
    decay_bias,
    decay_shift,
    head_gain,
    w_out,
    mlp_gain,
    mlp_up,
    mlp_down,
):
    rows_all = rms_rows(tokens, mixer_gain)
    gate_low = jnp.dot(rows_all, gate_down, preferred_element_type=jnp.float32).astype(jnp.bfloat16)
    joined = jnp.concatenate([w_query, w_key, w_value], axis=1)
    joined = lax.all_gather(joined, "fs", axis=0, tiled=True)
    sums = jnp.dot(rows_all, joined, preferred_element_type=jnp.float32).astype(jnp.bfloat16)
    wide = w_query.shape[1]
    query_sum, key_sum, value_sum = jnp.split(sums, (wide, 2 * wide), axis=1)
    mixer_out = mix_heads(
        query_sum,
        key_sum,
        value_sum,
        gate_low,
        gate_up,
        decay_bias,
        decay_shift,
        head_gain,
        1,
    )
    out_all = lax.all_gather(w_out, "fs", axis=0, tiled=True)
    mixer_term = times_transposed(mixer_out, out_all).astype(jnp.bfloat16).astype(jnp.float32)
    mixer_sum = lax.psum(mixer_term.astype(jnp.bfloat16), "tp").astype(jnp.float32)
    after_mixer = (tokens.astype(jnp.float32) + mixer_sum).astype(jnp.bfloat16)
    rows_two = rms_rows(after_mixer, mlp_gain)
    up_all, down_all = (
        lax.all_gather(mlp_up, "fs", axis=0, tiled=True),
        lax.all_gather(mlp_down, "fs", axis=0, tiled=True),
    )
    hidden = jnp.square(
        jax.nn.relu(jnp.dot(rows_two, up_all, preferred_element_type=jnp.float32))
    ).astype(jnp.bfloat16)
    mlp_term = times_transposed(hidden, down_all).astype(jnp.bfloat16).astype(jnp.float32)
    mlp_total = lax.psum(mlp_term.astype(jnp.bfloat16), "tp").astype(jnp.float32)
    return (after_mixer.astype(jnp.float32) + mlp_total).astype(jnp.bfloat16)


def solution(mesh):
    bands, cores = mesh.devices.shape
    fs = ("band", "share")
    split = Mesh(mesh.devices.reshape(bands // SHARE, SHARE, cores), fs + ("tp",))

    def layer(*arrays):
        heads = arrays[8].shape[1] // cores
        shared = cores == 2 and heads == SHARE and bands > 2 * SHARE
        axis = fs if shared else "fs"
        body = functools.partial(per_device_shared, SHARE) if shared else per_device
        row, both = P(axis, None), P(axis, "tp")
        return jax.shard_map(
            body,
            mesh=split if shared else mesh,
            in_specs=(
                row, P(), both, both, both, P(), P(None, "tp"), P("tp"), both, P("tp"),
                both, P(), both, both,
            ),
            out_specs=row,
            check_vma=False,
        )(*arrays)

    return layer
```
